32 devices in a mesh: kv: 4 (over y, x), tp: 8 (over z, core).
Axes of the slice: x: 2, y: 2, z: 4, core: 2. Of those that a mesh axis runs over, the one named last changes fastest.
Arguments:
- tokens: bfloat16 [64, 4096], P('tp', 'kv'), may hold values from -100 to 100
- state: float32 [64, 32, 128, 128], P('kv', 'tp'), may hold values from -3 to 3
- gain_pre: bfloat16 [4096], P('kv'), may hold values from 0.099609375 to 1.8984375
- w_gate_pre: bfloat16 [4096, 11264], P('kv', 'tp'), may hold values from -0.09375 to 0.09375
- w_up_pre: bfloat16 [4096, 11264], P('kv', 'tp'), may hold values from -0.09375 to 0.09375
- w_down_pre: bfloat16 [11264, 4096], P('tp', 'kv'), may hold values from -0.109375 to 0.109375
- gain_mix: bfloat16 [4096], P('kv'), may hold values from 0.099609375 to 1.8984375
- w_query: bfloat16 [4096, 4096], P('kv', 'tp'), may hold values from -0.09375 to 0.09375
- w_key: bfloat16 [4096, 4096], P('kv', 'tp'), may hold values from -0.09375 to 0.09375
- w_value: bfloat16 [4096, 4096], P('kv', 'tp'), may hold values from -0.09375 to 0.09375
- w_decay: bfloat16 [4096, 32], P('kv'), may hold values from -0.09375 to 0.09375
- w_blend: bfloat16 [4096, 32], P('kv'), may hold values from -0.09375 to 0.09375
- decay_base: float32 [32], P('tp'), may hold values from -3 to 0.7
- decay_shift: float32 [32], P('tp'), may hold values from -2 to 0.5
- head_gain: bfloat16 [128], replicated, may hold values from 0.099609375 to 1.8984375
- w_out: bfloat16 [4096, 4096], P('tp', 'kv'), may hold values from -0.09375 to 0.09375
- gain_post: bfloat16 [4096], P('kv'), may hold values from 0.099609375 to 1.8984375
- w_gate_post: bfloat16 [4096, 11264], P('kv', 'tp'), may hold values from -0.09375 to 0.09375
- w_up_post: bfloat16 [4096, 11264], P('kv', 'tp'), may hold values from -0.09375 to 0.09375
- w_down_post: bfloat16 [11264, 4096], P('tp', 'kv'), may hold values from -0.109375 to 0.109375
Outputs:
- result: bfloat16 [64, 4096], P('tp', 'kv')
- new_state: float32 [64, 32, 128, 128], P('kv', 'tp')
The draws below stay inside these ranges and needn't reach their ends.
All inputs are finite; a program needn't handle non-finite values.
Results may differ from the reference program's by a relative error of at most 0.015.
Values may be sent and summed in bfloat16 or wider, within the bound.
A program may use at most 64 MiB of HBM per device.

```python
import math
import jax
import jax.numpy as jnp
from jax import lax

D = 4096
FF = 11264
HEADS = 32
HEAD_DIM = 128
ROWS = 64
N_KV = 4
N_TP = 8


def draw_tokens(key, part):
    keys = jax.random.split(jax.random.fold_in(key, 11), 3)
    base = jnp.clip(jax.random.normal(keys[0], (ROWS, D), jnp.float32), -4.0, 4.0)
    rise_factor = 4.0
    low_end = 0.4
    high_end = 4.0
    row_scale = jnp.exp(jax.random.uniform(keys[1], (ROWS, 1), jnp.float32, math.log(low_end), math.log(high_end)))
    column_rise = jnp.exp(math.log(rise_factor) * jnp.arange(D, dtype=jnp.float32) / D)
    column_scale = column_rise * jax.random.uniform(keys[2], (D,), jnp.float32, 0.6, 1.4)
    return (base * row_scale * column_scale[None, :]).astype(jnp.bfloat16)


def block_levels(own_key, extent, cuts, smallest, high):
    loudness = 1.0
    for dim, shards_of in cuts:
        draws = jax.random.uniform(jax.random.fold_in(jax.random.fold_in(own_key, 6), dim), (shards_of,), jnp.float32, smallest / len(cuts), high / len(cuts))
        loudness = loudness * jnp.repeat(jnp.exp(draws), extent[dim] // shards_of).reshape((-1,) + (1,) * (len(extent) - 1 - dim))
    return loudness


def centred(stream_key, extent, width, limit, cuts=(), held_as=jnp.bfloat16):
    loudness = block_levels(stream_key, extent, cuts, -0.22, 0.18) if cuts else 1.0
    values = jax.random.normal(stream_key, extent, jnp.float32) * width * loudness
    return jnp.minimum(jnp.maximum(values, -limit), limit).astype(held_as)


def setup_inputs(seed: int = 0) -> dict:
    arg_keys = jax.random.split(jax.random.key(seed), 21)
    return {
        "tokens": draw_tokens(jax.random.fold_in(arg_keys[20], 71), 0),
        "state": centred(arg_keys[1], (ROWS, HEADS, HEAD_DIM, HEAD_DIM), 0.5, 3.0, ((0, 4), (1, 8)), jnp.float32),
        "gain_pre": jnp.clip(1.0 + 0.18 * jax.random.normal(arg_keys[2], (D,), jnp.float32), 0.099609375, 1.8984375).astype(jnp.bfloat16),
        "w_gate_pre": centred(arg_keys[3], (D, FF), D ** -0.5, 0.09375, ((0, 4), (1, 8))),
        "w_up_pre": centred(arg_keys[4], (D, FF), D ** -0.5, 0.09375, ((0, 4), (1, 8))),
        "w_down_pre": centred(arg_keys[5], (FF, D), (FF // 4) ** -0.5, 0.109375, ((0, 8), (1, 4))),
        "gain_mix": jnp.clip(1.0 + 0.18 * jax.random.normal(arg_keys[6], (D,), jnp.float32), 0.099609375, 1.8984375).astype(jnp.bfloat16),
        "w_query": centred(arg_keys[7], (D, HEADS * HEAD_DIM), D ** -0.5, 0.09375, ((0, 4), (1, 8))),
        "w_key": centred(arg_keys[8], (D, HEADS * HEAD_DIM), D ** -0.5, 0.09375, ((0, 4), (1, 8))),
        "w_value": centred(arg_keys[9], (D, HEADS * HEAD_DIM), D ** -0.5, 0.09375, ((0, 4), (1, 8))),
        "w_decay": centred(arg_keys[10], (D, HEADS), D ** -0.5, 0.09375, ((0, 4),)),
        "w_blend": centred(arg_keys[11], (D, HEADS), D ** -0.5, 0.09375, ((0, 4),)),
        "decay_base": jnp.clip(-3.0 + 3.7 * jax.random.uniform(arg_keys[12], (HEADS,), jnp.float32) ** block_levels(arg_keys[12], (HEADS,), ((0, 8),), -0.2, 0.2), -3.0, 0.7),
        "decay_shift": jnp.clip(-2.0 + 2.5 * jax.random.uniform(arg_keys[13], (HEADS,), jnp.float32) ** block_levels(arg_keys[13], (HEADS,), ((0, 8),), -0.2, 0.2), -2.0, 0.5),
        "head_gain": jnp.clip(1.0 + 0.18 * jax.random.normal(arg_keys[14], (HEAD_DIM,), jnp.float32), 0.099609375, 1.8984375).astype(jnp.bfloat16),
        "w_out": centred(arg_keys[15], (HEADS * HEAD_DIM, D), (HEADS * HEAD_DIM) ** -0.5, 0.09375, ((0, 8), (1, 4))),
        "gain_post": jnp.clip(1.0 + 0.18 * jax.random.normal(arg_keys[16], (D,), jnp.float32), 0.099609375, 1.8984375).astype(jnp.bfloat16),
        "w_gate_post": centred(arg_keys[17], (D, FF), D ** -0.5, 0.09375, ((0, 4), (1, 8))),
        "w_up_post": centred(arg_keys[18], (D, FF), D ** -0.5, 0.09375, ((0, 4), (1, 8))),
        "w_down_post": centred(arg_keys[19], (FF, D), (FF // 4) ** -0.5, 0.109375, ((0, 8), (1, 4))),
    }


EPS = 1e-06

def block_product(left, right, blocks):
    rows_all = left.shape[0]
    inner = left.shape[1] // blocks
    left_blocks = left.reshape(rows_all, blocks, inner).transpose(1, 0, 2)
    right_blocks = right.reshape(blocks, inner, right.shape[1])

    def add_block(running, pieces):
        product = jnp.dot(pieces[0], pieces[1], preferred_element_type=jnp.float32)
        rounded = lax.optimization_barrier(product.astype(jnp.bfloat16))
        return (running + rounded.astype(jnp.float32), None)
    start = jnp.zeros((rows_all, right.shape[1]), jnp.float32)
    running, unused = lax.scan(add_block, start, (left_blocks, right_blocks))
    return running

def inverse_rms(stream):
    values = stream.astype(jnp.float32)
    return lax.rsqrt(lax.optimization_barrier(jnp.mean(values * values, axis=1, keepdims=True)) + EPS)

def gained(stream, gain_vec):
    return (stream.astype(jnp.float32) * gain_vec.astype(jnp.float32)).astype(jnp.bfloat16)

def residual_add(stream, branch, weight):
    return (stream.astype(jnp.float32) + weight * branch).astype(jnp.bfloat16)

def unit_rows(values):
    return values * lax.rsqrt(lax.optimization_barrier(jnp.sum(values * values, axis=-1, keepdims=True)) + EPS)

def half_block(stream, gain_vec, w_gate, w_up, w_down):
    factor = inverse_rms(stream)
    scaled = gained(stream, gain_vec)
    gate_sum = factor * block_product(scaled, w_gate, N_KV)
    up_sum = factor * block_product(scaled, w_up, N_KV)
    hidden = (jax.nn.silu(gate_sum) * up_sum).astype(jnp.bfloat16)
    return block_product(hidden, w_down, N_TP)

def reference(tokens, state, gain_pre, w_gate_pre, w_up_pre, w_down_pre, gain_mix, w_query, w_key, w_value, w_decay, w_blend, decay_base, decay_shift, head_gain, w_out, gain_post, w_gate_post, w_up_post, w_down_post):
    first = residual_add(tokens, half_block(tokens, gain_pre, w_gate_pre, w_up_pre, w_down_pre), 0.5)
    factor = inverse_rms(first)
    scaled = gained(first, gain_mix)
    rows_all = first.shape[0]
    heads = state.shape[1]
    head_dim = state.shape[3]
    queries = (factor * block_product(scaled, w_query, N_KV)).reshape(rows_all, heads, head_dim)
    keys_new = (factor * block_product(scaled, w_key, N_KV)).reshape(rows_all, heads, head_dim)
    values_new = (factor * block_product(scaled, w_value, N_KV)).reshape(rows_all, heads, head_dim)
    decay_in = factor * block_product(scaled, w_decay, N_KV)
    blend_in = factor * block_product(scaled, w_blend, N_KV)
    queries = unit_rows(queries) * head_dim ** (-0.5)
    keys_unit = unit_rows(keys_new)
    log_rate = -jnp.exp(decay_base.astype(jnp.float32)) * jax.nn.softplus(decay_in + decay_shift.astype(jnp.float32))
    rate = jnp.exp(log_rate)
    beta = jax.nn.sigmoid(blend_in)
    recalled = jnp.einsum('bhk,bhkv->bhv', keys_unit, state, precision=lax.Precision.HIGHEST)
    correction = beta[:, :, None] * (values_new - rate[:, :, None] * recalled)
    new_state = rate[:, :, None, None] * state + keys_unit[:, :, :, None] * correction[:, :, None, :]
    read_out = jnp.einsum('bhk,bhkv->bhv', queries, new_state, precision=lax.Precision.HIGHEST)
    normed = read_out * lax.rsqrt(lax.optimization_barrier(jnp.mean(read_out * read_out, axis=2, keepdims=True)) + EPS)
    normed = (normed * head_gain.astype(jnp.float32)).astype(jnp.bfloat16).reshape(rows_all, heads * head_dim)
    second = residual_add(first, block_product(normed, w_out, N_TP), 1.0)
    result = residual_add(second, half_block(second, gain_post, w_gate_post, w_up_post, w_down_post), 0.5)
    return (result, new_state)
```

```python
import functools
from types import SimpleNamespace
from typing import Any, NamedTuple

import jax
import jax.numpy as jnp
from jax import lax
from jax.experimental import pallas as pl
from jax.experimental.pallas import tpu as pltpu
from jax.sharding import PartitionSpec as P

EPS = 1e-06
F32 = jnp.float32
BF16 = jnp.bfloat16
LANES = 128
OUT_STEP = 1024
MESH = pl.DeviceIdType.MESH


class Given(NamedTuple):
    tokens: Any
    state: Any
    gain_pre: Any
    w_gate_pre: Any
    w_up_pre: Any
    w_down_pre: Any
    gain_mix: Any
    w_query: Any
    w_key: Any
    w_value: Any
    w_decay: Any
    w_blend: Any
    decay_base: Any
    decay_shift: Any
    head_gain: Any
    w_out: Any
    gain_post: Any
    w_gate_post: Any
    w_up_post: Any
    w_down_post: Any


class Loads(NamedTuple):
    tokens: Any
    gain_pre: Any
    gain_mix: Any
    gain_post: Any
    head_gain: Any
    decay_base: Any
    decay_shift: Any
    w_gate_pre: Any
    w_up_pre: Any
    w_down_pre: Any
    w_decay: Any
    w_blend: Any
    w_key: Any
    w_query: Any
    w_value: Any
    state: Any
    w_out: Any
    w_gate_post: Any
    w_up_post: Any
    w_down_post: Any


NAMES = Given._fields
LOADS = Loads._fields
SMALL = LOADS[1:7]


def cuts(extent, step):
    return [(start, min(start + step, extent)) for start in range(0, extent, step)]


def layer_kernel(n_kv, n_tp, scratch_names, *refs):
    ins = Given(*refs[: len(NAMES)])
    result_ref, new_state_ref = refs[len(NAMES) : len(NAMES) + 2]
    s = SimpleNamespace(**dict(zip(scratch_names, refs[len(NAMES) + 2 :])))

    loads = Loads(
        *[
            pltpu.make_async_copy(getattr(ins, name), getattr(s, name), s.load_sem.at[i])
            for i, name in enumerate(LOADS)
        ]
    )
    first_loads = len(SMALL) + 3
    for copy in loads[:first_loads]:
        copy.start()

    kv = lax.axis_index("kv")
    tp = lax.axis_index("tp")
    own_count, chans = s.tokens.shape
    rows = own_count * n_tp
    seqs = rows // n_kv
    d_model = chans * n_kv
    wide = cuts(chans, OUT_STEP)

    def kv_peer(k):
        return lax.rem(kv + k, n_kv)

    def tp_peer(k):
        return lax.rem(tp + k, n_tp)

    barrier = pltpu.get_barrier_semaphore()
    for k in range(1, n_kv):
        pl.semaphore_signal(barrier, inc=1, device_id={"kv": kv_peer(k)}, device_id_type=MESH)
    for k in range(1, n_tp):
        pl.semaphore_signal(barrier, inc=1, device_id={"tp": tp_peer(k)}, device_id_type=MESH)
    pl.semaphore_wait(barrier, n_kv + n_tp - 2)

    sent = []

    def send(src, dst, phase, index, axis, peer):
        copy = pltpu.make_async_remote_copy(
            src_ref=src,
            dst_ref=dst,
            send_sem=getattr(s, phase + "_send").at[index],
            recv_sem=getattr(s, phase + "_recv").at[index],
            device_id={axis: peer},
            device_id_type=MESH,
        )
        copy.start()
        sent.append(copy)
        return copy

    def gather_rows(stream, phase, chunk, lo, hi):
        mine = stream.at[tp, :, lo:hi]
        return [
            send(mine, mine, phase, chunk * n_tp + k, "tp", tp_peer(k)) for k in range(1, n_tp)
        ]

    def gained_rows(stream, gain):
        values = stream[...].astype(F32).reshape(rows, chans)
        scaled = (values * s_small(gain)).astype(BF16)
        squares = values * values
        part = squares[:, :LANES]
        for lo in range(LANES, chans, LANES):
            part = part + squares[:, lo : lo + LANES]
        return scaled, part.reshape(n_kv, seqs, LANES)

    def s_small(name):
        return getattr(s, name)[...].astype(F32).reshape(1, -1)

    def spread_squares(part, phase):
        own, got = getattr(s, phase + "_own"), getattr(s, phase + "_got")
        own[...] = part
        return [
            send(own.at[kv_peer(k)], got.at[k], phase, k, "kv", kv_peer(k)) for k in range(1, n_kv)
        ]

    def inverse(copies, phase):
        for copy in copies:
            copy.wait_recv()
        total = getattr(s, phase + "_own")[kv]
        for k in range(1, n_kv):
            total = total + getattr(s, phase + "_got")[k]
        return lax.rsqrt(jnp.sum(total, axis=1, keepdims=True) / d_model + EPS)

    def settle_and_spread(left, weight_name, phase, base, share, stream_next, meanwhile=None):
        weight = getattr(s, weight_name)
        own, got = getattr(s, phase + "_own"), getattr(s, phase + "_got")
        moves = []
        for chunk, (lo, hi) in enumerate(wide):
            product = jnp.dot(left, weight[:, lo:hi], preferred_element_type=F32)
            own[:, :, lo:hi] = product.reshape(n_tp, own_count, hi - lo).astype(BF16)
            moves.append(
                [
                    send(
                        own.at[tp_peer(k), :, lo:hi],
                        got.at[k, :, lo:hi],
                        phase,
                        chunk * n_tp + k,
                        "tp",
                        tp_peer(k),
                    )
                    for k in range(1, n_tp)
                ]
            )
        if meanwhile is not None:
            meanwhile()
        spreads = []
        for chunk, (lo, hi) in enumerate(wide):
            for copy in moves[chunk]:
                copy.wait_recv()
            total = own[tp, :, lo:hi].astype(F32)
            for k in range(1, n_tp):
                total = total + got[k, :, lo:hi].astype(F32)
            fresh = (base(lo, hi) + share * total).astype(BF16)
            if stream_next is None:
                result_ref[:, lo:hi] = fresh
            else:
                getattr(s, stream_next)[tp, :, lo:hi] = fresh
                spreads += gather_rows(getattr(s, stream_next), stream_next, chunk, lo, hi)
        return spreads

    def half_block(stream_name, spreads, tag):
        for copy in spreads:
            copy.wait_recv()
        scaled, squares = gained_rows(getattr(s, stream_name), "gain_" + tag)
        square_moves = spread_squares(squares, "sq_" + tag)
        gate, up = getattr(s, "w_gate_" + tag), getattr(s, "w_up_" + tag)
        own, got, hidden = getattr(s, "gu_" + tag + "_own"), getattr(s, "gu_" + tag + "_got"), getattr(s, "hid_" + tag)
        columns = cuts(gate.shape[1], 512)
        getattr(loads, "w_gate_" + tag).wait()
        getattr(loads, "w_up_" + tag).wait()
        if tag == "pre":
            for copy in loads[first_loads:]:
                copy.start()
        moves = []
        for chunk, (lo, hi) in enumerate(columns):
            for side, weight in enumerate((gate, up)):
                product = jnp.dot(scaled, weight[:, lo:hi], preferred_element_type=F32)
                own[:, side, :, lo:hi] = product.astype(BF16).reshape(n_kv, seqs, hi - lo)
            moves.append(
                [
                    send(
                        own.at[kv_peer(k), :, :, lo:hi],
                        got.at[k, :, :, lo:hi],
                        "gu_" + tag,
                        chunk * n_kv + k,
                        "kv",
                        kv_peer(k),
                    )
                    for k in range(1, n_kv)
                ]
            )
        factor = inverse(square_moves, "sq_" + tag)
        spreads = []
        for chunk, (lo, hi) in enumerate(columns):
            for copy in moves[chunk]:
                copy.wait_recv()
            total = own[kv, :, :, lo:hi].astype(F32)
            for k in range(1, n_kv):
                total = total + got[k, :, :, lo:hi].astype(F32)
            gated = factor * total[0]
            value = gated * jax.nn.sigmoid(gated) * (factor * total[1])
            hidden[kv, :, lo:hi] = value.astype(BF16)
            mine = hidden.at[kv, :, lo:hi]
            spreads += [
                send(mine, mine, "hid_" + tag, chunk * n_kv + k, "kv", kv_peer(k))
                for k in range(1, n_kv)
            ]
        for copy in spreads:
            copy.wait_recv()
        getattr(loads, "w_down_" + tag).wait()
        return hidden[...].reshape(rows, gate.shape[1])

    loads.tokens.wait()
    s.stream_a[tp] = s.tokens[...]
    spreads = gather_rows(s.stream_a, "stream_a", 0, 0, chans)
    for copy in loads[1 : 1 + len(SMALL)]:
        copy.wait()
    hidden = half_block("stream_a", spreads, "pre")
    spreads = settle_and_spread(
        hidden,
        "w_down_pre",
        "rs_pre",
        lambda lo, hi: s.tokens[:, lo:hi].astype(F32),
        0.5,
        "stream_b",
    )

    for copy in spreads:
        copy.wait_recv()
    scaled, squares = gained_rows(s.stream_b, "gain_mix")
    square_moves = spread_squares(squares, "sq_mix")
    heads_all = s.w_decay.shape[0]
    loads.w_decay.wait()
    loads.w_blend.wait()
    for side, weight in enumerate((s.w_decay, s.w_blend)):
        product = lax.dot_general(
            scaled, weight[...], (((1,), (1,)), ((), ())), preferred_element_type=F32
        )
        s.db_own[:, side] = product.astype(BF16).reshape(n_kv, seqs, heads_all)
    db_moves = [
        send(s.db_own.at[kv_peer(k)], s.db_got.at[k], "db", k, "kv", kv_peer(k))
        for k in range(1, n_kv)
    ]
    width = s.w_key.shape[1]
    qkv_moves = []
    for side, name in enumerate(("w_key", "w_query", "w_value")):
        getattr(loads, name).wait()
        product = jnp.dot(scaled, getattr(s, name)[...], preferred_element_type=F32)
        s.qkv_own[:, side] = product.astype(BF16).reshape(n_kv, seqs, width)
        qkv_moves.append(
            [
                send(
                    s.qkv_own.at[kv_peer(k), side],
                    s.qkv_got.at[k, side],
                    "qkv",
                    side * n_kv + k,
                    "kv",
                    kv_peer(k),
                )
                for k in range(1, n_kv)
            ]
        )
    factor = inverse(square_moves, "sq_mix")
    for copy in db_moves:
        copy.wait_recv()
    gates = s.db_own[kv].astype(F32)
    for k in range(1, n_kv):
        gates = gates + s.db_got[k].astype(F32)
    state = s.state
    heads = state.shape[1]
    head_dim = state.shape[3]
    lane = lax.broadcasted_iota(jnp.int32, (seqs, heads_all), 1)
    for h in range(heads):
        chosen = lane == tp * heads + h
        decay_in = factor * jnp.sum(jnp.where(chosen, gates[0], 0.0), axis=1, keepdims=True)
        blend_in = factor * jnp.sum(jnp.where(chosen, gates[1], 0.0), axis=1, keepdims=True)
        base = jnp.broadcast_to(s.decay_base[:, h : h + 1], (seqs, head_dim))
        shifted = decay_in + jnp.broadcast_to(s.decay_shift[:, h : h + 1], (seqs, head_dim))
        soft = jnp.maximum(shifted, 0.0) + jnp.log1p(jnp.exp(-jnp.abs(shifted)))
        s.rate[h] = jnp.exp(-jnp.exp(base) * soft)
        s.beta[h] = jnp.broadcast_to(jax.nn.sigmoid(blend_in), (seqs, head_dim))

    def summed(side):
        for copy in qkv_moves[side]:
            copy.wait_recv()
        total = s.qkv_own[kv, side].astype(F32)
        for k in range(1, n_kv):
            total = total + s.qkv_got[k, side].astype(F32)
        return factor * total

    def unit(values):
        return values * lax.rsqrt(jnp.sum(values * values, axis=-1, keepdims=True) + EPS)

    keys = summed(0)
    queries = summed(1)
    stacked = [unit(keys[:, h * head_dim : (h + 1) * head_dim]) for h in range(heads)]
    stacked += [
        unit(queries[:, h * head_dim : (h + 1) * head_dim]) * head_dim ** (-0.5)
        for h in range(heads)
    ]
    for h in range(heads):
        s.key[h] = stacked[h]
        s.query[h] = stacked[heads + h]
    values_new = summed(2)
    loads.state.wait()

    place = lax.broadcasted_iota(jnp.int32, (8, head_dim), 0)

    def recall(b, carry):
        at = pl.ds(b, 1)
        for h in range(heads):
            pair = jnp.where(
                place == 0, s.key[h, at, :], jnp.where(place == 1, s.query[h, at, :], 0.0)
            )
            answer = jnp.dot(
                pair, state[b, h], preferred_element_type=F32, precision=lax.Precision.HIGHEST
            )
            s.recalled[h, at, :] = answer[0:1]
            s.past[h, at, :] = answer[1:2]
        return carry

    lax.fori_loop(0, seqs, recall, 0, unroll=4)
    for h in range(heads):
        value = values_new[:, h * head_dim : (h + 1) * head_dim]
        correction = s.beta[h] * (value - s.rate[h] * s.recalled[h])
        s.correction[h] = correction
        overlap = jnp.sum(stacked[h] * stacked[heads + h], axis=1, keepdims=True)
        read = s.rate[h] * s.past[h] + overlap * correction
        normed = read * lax.rsqrt(jnp.mean(read * read, axis=1, keepdims=True) + EPS)
        normed = normed * s_small("head_gain")
        s.normed[kv, :, h * head_dim : (h + 1) * head_dim] = normed.astype(BF16)
    store = pltpu.make_async_copy(state, new_state_ref, s.store_sem.at[0])

    def update_state():
        turned_keys = stacked[:heads]
        left_over = LANES - heads * seqs
        if left_over:
            turned_keys = turned_keys + [jnp.zeros((left_over, head_dim), F32)]
        s.columns[...] = jnp.concatenate(turned_keys, axis=0).T

        def one_sequence(b, carry):
            turned = pltpu.roll(s.columns[...], lax.rem(LANES - b, LANES), 1)
            at = pl.ds(b, 1)
            for h in range(heads):
                key = turned[:, h * seqs : h * seqs + 1]
                state[b, h] = s.rate[h, at, :] * state[b, h] + key * s.correction[h, at, :]
            return carry

        lax.fori_loop(0, seqs, one_sequence, 0)
        store.start()

    mine = s.normed.at[kv]
    spreads = [send(mine, mine, "normed", k, "kv", kv_peer(k)) for k in range(1, n_kv)]
    for copy in spreads:
        copy.wait_recv()
    loads.w_out.wait()
    spreads = settle_and_spread(
        s.normed[...].reshape(rows, width),
        "w_out",
        "rs_mix",
        lambda lo, hi: s.stream_b[tp, :, lo:hi].astype(F32),
        1.0,
        "stream_c",
        update_state,
    )

    hidden = half_block("stream_c", spreads, "post")
    settle_and_spread(
        hidden,
        "w_down_post",
        "rs_post",
        lambda lo, hi: s.stream_c[tp, :, lo:hi].astype(F32),
        0.5,
        None,
    )
    for copy in sent:
        copy.wait_send()
    store.wait()


def output_kernel(result_in, state_in, result_out, state_out, rows, held, in_sem, out_sem):
    pieces = [(result_in, rows, result_out)]
    step = 2 if held.shape[0] % 2 == 0 else 1
    for b in range(0, held.shape[0], step):
        at = pl.ds(b, step)
        pieces.append((state_in.at[at], held.at[at], state_out.at[at]))
    taken = [
        pltpu.make_async_copy(source, middle, in_sem.at[i])
        for i, (source, middle, target) in enumerate(pieces)
    ]
    for copy in taken:
        copy.start()
    given_out = []
    for i, (source, middle, target) in enumerate(pieces):
        taken[i].wait()
        copy = pltpu.make_async_copy(middle, target, out_sem.at[i])
        copy.start()
        given_out.append(copy)
    for copy in given_out:
        copy.wait()


def on_device(n_kv, n_tp, *args):
    given = SimpleNamespace(**dict(zip(NAMES, args)))
    own_count, chans = given.tokens.shape
    rows = own_count * n_tp
    seqs = rows // n_kv
    ff = given.w_gate_pre.shape[1]
    width = given.w_query.shape[1]
    heads, head_dim = given.state.shape[1], given.state.shape[3]
    given.w_decay, given.w_blend = given.w_decay.T, given.w_blend.T
    given.decay_base = given.decay_base.reshape(1, -1)
    given.decay_shift = given.decay_shift.reshape(1, -1)
    heads_all = given.w_decay.shape[0]
    out_steps = len(cuts(chans, OUT_STEP))
    ff_steps = len(cuts(ff, 512))
    scratch = {name: pltpu.VMEM(getattr(given, name).shape, getattr(given, name).dtype) for name in LOADS}
    scratch["load_sem"] = pltpu.SemaphoreType.DMA((len(LOADS),))
    scratch["store_sem"] = pltpu.SemaphoreType.DMA((1,))

    def semaphores(phase, count):
        scratch[phase + "_send"] = pltpu.SemaphoreType.DMA((count,))
        scratch[phase + "_recv"] = pltpu.SemaphoreType.DMA((count,))

    for name in ("stream_a", "stream_b", "stream_c"):
        scratch[name] = pltpu.VMEM((n_tp, own_count, chans), BF16)
        semaphores(name, n_tp * out_steps)
    for tag in ("pre", "post", "mix"):
        scratch["sq_" + tag + "_own"] = pltpu.VMEM((n_kv, seqs, LANES), F32)
        scratch["sq_" + tag + "_got"] = pltpu.VMEM((n_kv, seqs, LANES), F32)
        semaphores("sq_" + tag, n_kv)
        scratch["rs_" + tag + "_own"] = pltpu.VMEM((n_tp, own_count, chans), BF16)
        scratch["rs_" + tag + "_got"] = pltpu.VMEM((n_tp, own_count, chans), BF16)
        semaphores("rs_" + tag, n_tp * out_steps)
    for tag in ("pre", "post"):
        scratch["gu_" + tag + "_own"] = pltpu.VMEM((n_kv, 2, seqs, ff), BF16)
        scratch["gu_" + tag + "_got"] = pltpu.VMEM((n_kv, 2, seqs, ff), BF16)
        semaphores("gu_" + tag, n_kv * ff_steps)
        scratch["hid_" + tag] = pltpu.VMEM((n_kv, seqs, ff), BF16)
        semaphores("hid_" + tag, n_kv * ff_steps)
    for name in ("db_own", "db_got"):
        scratch[name] = pltpu.VMEM((n_kv, 2, seqs, heads_all), BF16)
    semaphores("db", n_kv)
    for name in ("qkv_own", "qkv_got"):
        scratch[name] = pltpu.VMEM((n_kv, 3, seqs, width), BF16)
    semaphores("qkv", 3 * n_kv)
    for name in ("rate", "beta", "key", "query", "recalled", "past", "correction"):
        scratch[name] = pltpu.VMEM((heads, seqs, head_dim), F32)
    scratch["columns"] = pltpu.VMEM((head_dim, LANES), F32)
    scratch["normed"] = pltpu.VMEM((n_kv, seqs, width), BF16)
    semaphores("normed", n_kv)

    anywhere = pl.BlockSpec(memory_space=pl.ANY)
    in_vmem = pl.BlockSpec(memory_space=pltpu.VMEM)
    out_shape = (
        jax.ShapeDtypeStruct(given.tokens.shape, BF16),
        jax.ShapeDtypeStruct(given.state.shape, F32),
    )
    result, new_state = pl.pallas_call(
        functools.partial(layer_kernel, n_kv, n_tp, tuple(scratch)),
        out_shape=out_shape,
        in_specs=[anywhere] * len(NAMES),
        out_specs=(in_vmem, anywhere),
        scratch_shapes=list(scratch.values()),
        compiler_params=pltpu.CompilerParams(collective_id=0, has_side_effects=True),
    )(*[getattr(given, name) for name in NAMES])
    return pl.pallas_call(
        output_kernel,
        out_shape=out_shape,
        in_specs=[anywhere, anywhere],
        out_specs=(anywhere, anywhere),
        scratch_shapes=[
            pltpu.VMEM(given.tokens.shape, BF16),
            pltpu.VMEM(given.state.shape, F32),
            pltpu.SemaphoreType.DMA((seqs + 1,)),
            pltpu.SemaphoreType.DMA((seqs + 1,)),
        ],
    )(result, new_state)


def solution(mesh):
    return jax.shard_map(
        functools.partial(on_device, mesh.shape["kv"], mesh.shape["tp"]),
        mesh=mesh,
        in_specs=(
            P("tp", "kv"),
            P("kv", "tp", None, None),
            P("kv"),
            P("kv", "tp"),
            P("kv", "tp"),
            P("tp", "kv"),
            P("kv"),
            P("kv", "tp"),
            P("kv", "tp"),
            P("kv", "tp"),
            P("kv", None),
            P("kv", None),
            P("tp"),
            P("tp"),
            P(),
            P("tp", "kv"),
            P("kv"),
            P("kv", "tp"),
            P("kv", "tp"),
            P("tp", "kv"),
        ),
        out_specs=(P("tp", "kv"), P("kv", "tp", None, None)),
        check_vma=False,
    )
```
